32 devices in a mesh: ep: 8 (over z, x), tp: 4 (over y, core).
Axes of the slice: x: 2, y: 2, z: 4, core: 2. Of those that a mesh axis runs over, the one named last changes fastest.
Arguments:
- tokens: bfloat16 [2048, 2048], P('ep'), may hold values from -6 to 6
- routes: int32 [2048, 4], P('ep'), may hold values from 0 to 7, all different within a row; in each aligned block of 256 rows (0 to 255, 256 to 511, ...) at most 160 rows name the same one
- gate_weights: float32 [2048, 4], P('ep'), may hold values from 0.05 to 1
- out_grad: bfloat16 [2048, 2048], P('ep'), may hold values from -0.59765625 to 0.59765625
- w_gate: bfloat16 [8, 2048, 1024], P('ep', None, 'tp'), may hold values from -0.1875 to 0.1875
- w_up: bfloat16 [8, 2048, 1024], P('ep', None, 'tp'), may hold values from -0.1875 to 0.1875
- w_down: bfloat16 [8, 1024, 2048], P('ep', 'tp'), may hold values from -0.1875 to 0.1875
Outputs:
- token_grad: bfloat16 [2048, 2048], P('ep', 'tp')
- gate_grad: float32 [2048, 4], P('ep')
- gate_weight_grad: float32 [8, 2048, 1024], P('ep', None, 'tp')
- up_weight_grad: float32 [8, 2048, 1024], P('ep', None, 'tp')
- down_weight_grad: float32 [8, 1024, 2048], P('ep', 'tp')
The draws below stay inside these ranges and needn't reach their ends.
Inputs may be any that keep to these rules, and one draw needn't show every extreme that they name: `routes`: each row names 4 different experts. In each aligned block of 256 rows (the rows of one device) no expert is named by more than 160 rows, and in some block an expert is named by exactly 160 rows.
All inputs are finite; a program needn't handle non-finite values.
Results may differ from the reference program's by a relative error of at most 0.012.
Values may be sent and summed in bfloat16 or wider, within the bound.
A program may use at most 128 MiB of HBM per device.

```python
import math
import jax
import jax.numpy as jnp
import numpy as np
from jax import lax

D = 2048
FF = 1024
TOPK = 4
TOK_DEV = 256
EXPERTS = 8
TOKENS = 2048
CAP = 160
N_EP = 8
N_TP = 4


def steps_of(rng, extent, split, smallest, high):
    def one(axis_at, parts):
        heights = jax.random.uniform(jax.random.fold_in(jax.random.fold_in(rng, 6), axis_at), (parts,), jnp.float32, smallest / len(split), high / len(split))
        return jnp.repeat(jnp.exp(heights), extent[axis_at] // parts).reshape((-1,) + (1,) * (len(extent) - axis_at - 1))

    gain = one(*split[0])
    for cut in split[1:]:
        gain = gain * one(*cut)
    return gain


def assign_block(key, own, number, rows, amount, top, reach, lean):
    ranking = jax.random.permutation(key, amount)
    crowded, usual = portions_of(amount, rows * top, reach, lean, True), portions_of(amount, rows * top, reach, lean, False)
    places = jnp.arange(amount)

    def named(sizes, rotation):
        used = int((sizes > 0).sum())
        fixed = max(1, used // 4)
        moved = fixed + (places - fixed + rotation * (used - fixed)) % max(1, amount - fixed)
        return jnp.zeros((amount,), jnp.int32).at[ranking[jnp.where(places < fixed, places, moved)]].set(jnp.asarray(sizes, jnp.int32))

    sizes = jnp.where(number % 4 == 0, named(crowded, number // 4), named(usual, number - number // 4 - 1))
    mixed = jax.random.permutation(jax.random.fold_in(own, 3), amount)
    source_of, receiver = mixed[0:amount // 2 * 2:2], mixed[1:amount // 2 * 2:2]
    margin = jnp.minimum(sizes[source_of] - 1, reach - sizes[receiver]) // 2
    margin = jnp.where((source_of == ranking[0]) | (receiver == ranking[0]) | (sizes[receiver] == 0), 0, jnp.maximum(margin, 0))
    moved = jax.random.randint(jax.random.fold_in(own, 4), (amount // 2,), 0, 1 << 20) % (margin + 1)
    sizes = sizes.at[source_of].add(-moved).at[receiver].add(moved)
    labels = jnp.searchsorted(jnp.cumsum(sizes), jnp.arange(rows * top), side="right").astype(jnp.int32)
    grid = labels.reshape(top, rows).T
    grid = grid[jax.random.permutation(jax.random.fold_in(own, 1), rows)]
    rotation = jax.random.randint(jax.random.fold_in(own, 2), (rows, 1), 0, top)
    return jnp.take_along_axis(grid, (jnp.arange(top)[None, :] + rotation) % top, axis=1)


def portions_of(count, total, reach, lean, full):
    weights = [(1 << 20) // math.isqrt(rank ** lean) + 1 for rank in range(1, count + 1)]
    largest = reach if full else min(reach, max(-(-total // count), total * weights[0] // sum(weights)))
    least = 1 if total - largest >= count - 1 else 0
    given, surplus = [largest] + [least] * (count - 1), total - largest - least * (count - 1)
    while surplus > 0:
        movable = [i for i in range(1, count) if given[i] < largest] or [i for i in range(1, count) if given[i] < reach]
        mass, remaining = sum([weights[i] for i in movable]), surplus
        for i in movable:
            more = min(reach - given[i], max(1, remaining * weights[i] // mass), surplus)
            given[i] = given[i] + more
            surplus = surplus - more
    return np.array(given)


def bell_draw(key, extent, scale, bound, shards=(), kind=jnp.bfloat16):
    values = jax.random.normal(key, extent, jnp.float32) * scale
    if len(shards) > 0:
        values = steps_of(key, extent, shards, -0.22, 0.18) * values
    return jnp.clip(values, min=-bound, max=bound).astype(kind)


def setup_inputs(seed: int = 0) -> dict:
    key_of = jax.random.split(jax.random.key(seed), 8)
    tokens = bell_draw(key_of[0], (TOKENS, D), 1.0, 6.0, ((0, 8),))
    routes_keys = jax.random.split(jax.random.fold_in(key_of[1], 1), TOKENS // TOK_DEV)
    routes_turns = jax.random.permutation(jax.random.fold_in(key_of[1], 3), TOKENS // TOK_DEV)
    routes = jax.vmap(lambda own, number: assign_block(jax.random.fold_in(key_of[1], 2), own, number, TOK_DEV, EXPERTS, TOPK, CAP, 1))(routes_keys, routes_turns).reshape((TOKENS, TOPK))
    gate_weights = jnp.clip(jnp.exp(math.log(1.0) - 2.9957323 * jax.random.uniform(key_of[2], (TOKENS, TOPK), jnp.float32) ** steps_of(key_of[2], (TOKENS, TOPK), ((0, 8),), -0.2, 0.2)), 0.05, 1.0)
    out_grad = bell_draw(key_of[3], (TOKENS, D), 0.1, 0.59765625, ((0, 8),))
    w_gate = bell_draw(key_of[4], (EXPERTS, D, FF), (D // 2) ** -0.5, 0.1875, ((0, 8), (2, 4)))
    w_up = bell_draw(key_of[5], (EXPERTS, D, FF), (D // 2) ** -0.5, 0.1875, ((0, 8), (2, 4)))
    w_down = bell_draw(key_of[6], (EXPERTS, FF, D), FF ** -0.5, 0.1875, ((0, 8), (1, 4)))
    return dict(tokens=tokens, routes=routes, gate_weights=gate_weights, out_grad=out_grad, w_gate=w_gate, w_up=w_up, w_down=w_down)


clamp_limit = 7.0
sigmoid_slope = 1.702


def unit_backward(gate_pre, up_pre, hidden_grad):
    glu = jnp.minimum(gate_pre, clamp_limit)
    linear = jnp.clip(up_pre, -clamp_limit, clamp_limit)
    sigma = jax.nn.sigmoid(sigmoid_slope * glu)
    active = glu * sigma
    hidden = (active * (linear + 1.0)).astype(jnp.bfloat16)
    slope_term = sigma + sigmoid_slope * active * (1.0 - sigma)
    gate_pre_grad = jnp.where(gate_pre < clamp_limit, hidden_grad * (linear + 1.0) * slope_term, 0.0).astype(jnp.bfloat16)
    up_pre_grad = jnp.where(jnp.abs(up_pre) < clamp_limit, hidden_grad * active, 0.0).astype(jnp.bfloat16)
    return hidden, gate_pre_grad, up_pre_grad


def block_round_total(partial_value):
    rounded = lax.optimization_barrier(partial_value.astype(jnp.bfloat16))
    return jnp.sum(rounded.astype(jnp.float32), axis=0)


def reference(tokens, routes, gate_weights, out_grad, w_gate, w_up, w_down):
    blocks = routes.reshape(N_EP, TOK_DEV * TOPK)
    onehot = (blocks[:, :, None] == jnp.arange(EXPERTS, dtype=jnp.int32)[None, None, :]).astype(jnp.int32)
    slot_rank = jnp.sum((jnp.cumsum(onehot, axis=1) - onehot) * onehot, axis=2)
    source = jnp.arange(N_EP, dtype=jnp.int32)[:, None]
    target = (blocks * (N_EP * CAP) + source * CAP + slot_rank).reshape(-1)
    pair_index = jnp.arange(TOKENS * TOPK, dtype=jnp.int32)
    pair_table = jnp.zeros((EXPERTS * N_EP * CAP,), jnp.int32).at[target].set(pair_index)
    filled = jnp.zeros((EXPERTS * N_EP * CAP,), jnp.int32).at[target].set(1)
    flat_weights = gate_weights.reshape(-1)
    row_count = N_EP * CAP

    def per_expert(running, expert):
        token_acc, gate_acc = running
        slot_pairs = lax.dynamic_slice_in_dim(pair_table, expert * row_count, row_count)
        is_live = lax.dynamic_slice_in_dim(filled, expert * row_count, row_count)[:, None] > 0
        token_index = slot_pairs // TOPK
        x_rows = jnp.where(is_live, tokens[token_index], jnp.zeros((), jnp.bfloat16))
        dy_rows = out_grad[token_index]
        scaled = jnp.where(is_live, flat_weights[slot_pairs][:, None] * dy_rows.astype(jnp.float32), 0.0).astype(jnp.bfloat16)
        gate_mat = w_gate[expert]
        up_mat = w_up[expert]
        down_mat = w_down[expert]
        gate_pre = jnp.dot(x_rows, gate_mat, preferred_element_type=jnp.float32)
        up_pre = jnp.dot(x_rows, up_mat, preferred_element_type=jnp.float32)
        hidden_grad = jnp.dot(scaled, down_mat.T, preferred_element_type=jnp.float32)
        hidden, gate_pre_grad, up_pre_grad = unit_backward(gate_pre, up_pre, hidden_grad)
        unit_block = FF // N_TP
        gate_blocks = gate_pre_grad.astype(jnp.float32).reshape(row_count, N_TP, unit_block)
        up_blocks = up_pre_grad.astype(jnp.float32).reshape(row_count, N_TP, unit_block)
        hidden_blocks = hidden.astype(jnp.float32).reshape(row_count, N_TP, unit_block)
        gate_mat_blocks = gate_mat.astype(jnp.float32).reshape(D, N_TP, unit_block)
        up_mat_blocks = up_mat.astype(jnp.float32).reshape(D, N_TP, unit_block)
        down_blocks = down_mat.astype(jnp.float32).reshape(N_TP, unit_block, D)
        row_partial = jnp.einsum('rnf,dnf->nrd', gate_blocks, gate_mat_blocks) + jnp.einsum('rnf,dnf->nrd', up_blocks, up_mat_blocks)
        row_grad = block_round_total(row_partial).astype(jnp.bfloat16)
        expert_out = block_round_total(jnp.einsum('rnf,nfd->nrd', hidden_blocks, down_blocks))
        token_acc = token_acc.at[token_index].add(jnp.where(is_live, row_grad.astype(jnp.float32), 0.0))
        products = jnp.sum(dy_rows.astype(jnp.float32) * expert_out, axis=1)
        gate_acc = gate_acc.at[slot_pairs].add(jnp.where(is_live[:, 0], products, 0.0))
        gate_weight_grad = jnp.dot(x_rows.T, gate_pre_grad, preferred_element_type=jnp.float32)
        up_weight_grad = jnp.dot(x_rows.T, up_pre_grad, preferred_element_type=jnp.float32)
        down_weight_grad = jnp.dot(hidden.T, scaled, preferred_element_type=jnp.float32)
        return (token_acc, gate_acc), (gate_weight_grad, up_weight_grad, down_weight_grad)

    start = (jnp.zeros((TOKENS, D), jnp.float32), jnp.zeros((TOKENS * TOPK,), jnp.float32))
    (token_acc, gate_acc), grads = lax.scan(per_expert, start, jnp.arange(EXPERTS, dtype=jnp.int32))
    return (token_acc.astype(jnp.bfloat16), gate_acc.reshape(TOKENS, TOPK), grads[0], grads[1], grads[2])
```

```python
import jax
import jax.numpy as jnp
from jax import lax
from jax.experimental import pallas as pl
from jax.experimental.pallas import tpu as pltpu
from jax.sharding import PartitionSpec as P

clamp_limit = 7.0
sigmoid_slope = 1.702
MESH = pl.DeviceIdType.MESH


def partners():
    ep_count = lax.axis_size("ep")
    tp_count = lax.axis_size("tp")
    here = lax.axis_index("ep")
    part = lax.axis_index("tp")
    beside = part + 1 - 2 * (part % 2)
    across = (part + tp_count // 2) % tp_count
    return ep_count, here, part, beside, across


def greet(ep_count, here, part, beside, across):
    barrier = pltpu.get_barrier_semaphore()
    pl.semaphore_signal(barrier, inc=1, device_id=(here, beside), device_id_type=MESH)
    pl.semaphore_signal(barrier, inc=1, device_id=(here, across), device_id_type=MESH)

    def call(j, carry):
        peer = (here + j) % ep_count
        pl.semaphore_signal(barrier, inc=1, device_id=(peer, part), device_id_type=MESH)
        return carry

    lax.fori_loop(1, ep_count, call, 0)
    pl.semaphore_wait(barrier, ep_count + 1)


def remote(src, dst, sent, got, device):
    return pltpu.make_async_remote_copy(
        src_ref=src, dst_ref=dst, send_sem=sent, recv_sem=got, device_id=device, device_id_type=MESH
    )


def dispatch_kernel(
    send_ref, weight_ref, rows_ref, weights_out, s1, r1, s2, r2, s3, r3, s4, r4, sw, rw, own_sem
):
    ep_count, here, part, beside, across = partners()
    width = send_ref.shape[3]

    def block(source, owner):
        columns = pl.ds(pl.multiple_of(owner * width, width), width)
        return rows_ref.at[:, source, :, columns]

    greet(ep_count, here, part, beside, across)

    def first(j):
        peer = (here + j) % ep_count
        return remote(send_ref.at[:, peer], block(here, part), s1.at[j], r1.at[j], (peer, part))

    def first_weight(j):
        peer = (here + j) % ep_count
        return remote(
            weight_ref.at[peer], weights_out.at[here], sw.at[j], rw.at[j], (peer, part)
        )

    def near(j):
        source = (here + ep_count - j) % ep_count
        return remote(block(source, part), block(source, part), s2.at[j], r2.at[j], (here, beside))

    def far(j):
        source = (here + ep_count - j) % ep_count
        return remote(block(source, part), block(source, part), s3.at[j], r3.at[j], (here, across))

    def onward(j):
        source = (here + ep_count - j) % ep_count
        return remote(
            block(source, across), block(source, across), s4.at[j], r4.at[j], (here, beside)
        )

    own = pltpu.make_async_copy(send_ref.at[:, here], block(here, part), own_sem.at[0])
    own_weight = pltpu.make_async_copy(weight_ref.at[here], weights_out.at[here], own_sem.at[1])
    own.start()
    own_weight.start()

    def launch(j, carry):
        first_weight(j).start()
        first(j).start()
        return carry

    lax.fori_loop(1, ep_count, launch, 0)
    own.wait()
    far(0).start()
    near(0).start()

    def pass_on(j, carry):
        @pl.when(j < ep_count)
        def _():
            first(j).wait_recv()
            far(j).start()
            near(j).start()

        @pl.when(j >= 2)
        def _():
            far(j - 2).wait_recv()
            onward(j - 2).start()

        return carry

    lax.fori_loop(1, ep_count + 2, pass_on, 0)
    own_weight.wait()

    def finish(j, carry):
        near(j).wait()
        onward(j).wait()
        far(j).wait_send()

        @pl.when(j >= 1)
        def _():
            first(j).wait_send()
            first_weight(j).wait()

        return carry

    lax.fori_loop(0, ep_count, finish, 0)


def dispatch(send, weights, model_width):
    _, ep_count, capacity, width = send.shape
    sems = [pltpu.SemaphoreType.DMA((ep_count,)) for _ in range(10)]
    return pl.pallas_call(
        dispatch_kernel,
        out_shape=(
            jax.ShapeDtypeStruct((2, ep_count, capacity, model_width), jnp.bfloat16),
            jax.ShapeDtypeStruct(weights.shape, jnp.float32),
        ),
        in_specs=[pl.BlockSpec(memory_space=pltpu.VMEM)] * 2,
        out_specs=(pl.BlockSpec(memory_space=pl.ANY), pl.BlockSpec(memory_space=pltpu.VMEM)),
        scratch_shapes=sems + [pltpu.SemaphoreType.DMA((2,))],
        compiler_params=pltpu.CompilerParams(collective_id=0, has_side_effects=True),
    )(send, weights)


def combine_kernel(
    rows_ref, product_ref, back_ref, back_product, near_buf, far_send, far_buf, last_send,
    product_near, product_sum, product_far, product_send,
    s1, r1, s2, r2, s3, r3, sw, rw, small_send, small_recv,
):
    ep_count, here, part, beside, across = partners()
    width = back_ref.shape[2]
    beside_far = (beside + lax.axis_size("tp") // 2) % lax.axis_size("tp")

    def columns(owner):
        return pl.ds(pl.multiple_of(owner * width, width), width)

    greet(ep_count, here, part, beside, across)

    def near(which, j):
        target = (here + j) % ep_count
        owner = beside_far if which == 0 else beside
        return remote(
            rows_ref.at[target, :, columns(owner)], near_buf.at[which, j],
            s1.at[which, j], r1.at[which, j], (here, beside),
        )

    def far(j):
        return remote(far_send.at[j], far_buf.at[j], s2.at[j], r2.at[j], (here, across))

    def last(j):
        peer = (here + j) % ep_count
        return remote(last_send.at[j], back_ref.at[here], s3.at[j], r3.at[j], (peer, part))

    def last_product(j):
        peer = (here + j) % ep_count
        return remote(
            product_send.at[peer], back_product.at[here], sw.at[j], rw.at[j], (peer, part)
        )

    small_near = remote(product_ref, product_near, small_send.at[0], small_recv.at[0], (here, beside))
    small_far = remote(product_sum, product_far, small_send.at[1], small_recv.at[1], (here, across))
    small_near.start()

    def launch(j, carry):
        near(0, j).start()
        near(1, j).start()
        return carry

    lax.fori_loop(0, ep_count, launch, 0)
    small_near.wait_recv()
    product_sum[...] = product_ref[...] + product_near[...]
    small_far.start()

    def middle(j, carry):
        near(0, j).wait_recv()
        target = (here + j) % ep_count
        mine = rows_ref[target, :, columns(across)].astype(jnp.float32)
        far_send[j] = (mine + near_buf[0, j].astype(jnp.float32)).astype(jnp.bfloat16)
        far(j).start()
        return carry

    lax.fori_loop(0, ep_count, middle, 0)
    small_far.wait_recv()
    product_send[...] = product_sum[...] + product_far[...]

    def total(j):
        near(1, j).wait_recv()
        far(j).wait_recv()
        target = (here + j) % ep_count
        mine = rows_ref[target, :, columns(part)].astype(jnp.float32)
        added = mine + near_buf[1, j].astype(jnp.float32) + far_buf[j].astype(jnp.float32)
        return added.astype(jnp.bfloat16)

    def end(j, carry):
        last_send[j] = total(j)
        last(j).start()
        last_product(j).start()
        return carry

    back_ref[here] = total(0)
    back_product[here] = product_send[here]
    lax.fori_loop(1, ep_count, end, 0)

    small_near.wait_send()
    small_far.wait_send()

    def finish(j, carry):
        near(0, j).wait_send()
        near(1, j).wait_send()
        far(j).wait_send()

        @pl.when(j >= 1)
        def _():
            last(j).wait()
            last_product(j).wait()

        return carry

    lax.fori_loop(0, ep_count, finish, 0)


def combine(rows, products, width):
    ep_count, capacity, _ = rows.shape
    one = (ep_count, capacity, width)
    small = pltpu.VMEM(products.shape, jnp.float32)
    dma = pltpu.SemaphoreType.DMA
    return pl.pallas_call(
        combine_kernel,
        out_shape=(
            jax.ShapeDtypeStruct(one, jnp.bfloat16),
            jax.ShapeDtypeStruct(products.shape, jnp.float32),
        ),
        in_specs=[pl.BlockSpec(memory_space=pltpu.VMEM)] * 2,
        out_specs=(pl.BlockSpec(memory_space=pltpu.VMEM),) * 2,
        scratch_shapes=[
            pltpu.VMEM((2,) + one, jnp.bfloat16),
            pltpu.VMEM(one, jnp.bfloat16),
            pltpu.VMEM(one, jnp.bfloat16),
            pltpu.VMEM(one, jnp.bfloat16),
            small, small, small, small,
            dma((2, ep_count)), dma((2, ep_count)),
            dma((ep_count,)), dma((ep_count,)), dma((ep_count,)), dma((ep_count,)),
            dma((ep_count,)), dma((ep_count,)), dma((2,)), dma((2,)),
        ],
        compiler_params=pltpu.CompilerParams(
            collective_id=1, has_side_effects=True, vmem_limit_bytes=48 * 1024 * 1024
        ),
    )(rows, products)


def local(tokens, routes, gate_weights, out_grad, w_gate, w_up, w_down):
    f32, bf16 = jnp.float32, jnp.bfloat16
    ep_count = lax.axis_size("ep")
    tp_count = lax.axis_size("tp")
    part = lax.axis_index("tp")
    token_count, model_width = tokens.shape
    top_count = routes.shape[1]
    experts = ep_count * w_gate.shape[0]
    capacity = token_count * top_count * 5 // (4 * experts)
    width = model_width // tp_count

    match = routes[:, :, None] == jnp.arange(experts, dtype=jnp.int32)[None, None, :]
    named = jnp.any(match, axis=1)
    before = jnp.arange(token_count)[:, None] > jnp.arange(token_count)[None, :]
    rank = jnp.dot(before.astype(bf16), named.astype(bf16), preferred_element_type=f32)
    rank = jnp.where(named, rank.astype(jnp.int32), -1)
    pick = rank.T[:, None, :] == jnp.arange(capacity, dtype=jnp.int32)[None, :, None]
    pick_flat = pick.reshape(experts * capacity, token_count).astype(bf16)
    weight_of = jnp.sum(jnp.where(match, gate_weights[:, :, None], 0.0), axis=1)
    send_weights = jnp.sum(jnp.where(pick, weight_of.T[:, None, :], 0.0), axis=2)
    own = jnp.stack(
        [lax.dynamic_slice_in_dim(a, part * width, width, 1) for a in (tokens, out_grad)]
    )
    send = jnp.einsum("rt,atw->arw", pick_flat, own, preferred_element_type=f32).astype(bf16)
    send = send.reshape(2, experts, capacity, width)

    both, weights = dispatch(send, send_weights[:, None, :], model_width)
    row_count = ep_count * capacity
    x_rows = both[0].reshape(row_count, model_width)
    dy_rows = both[1].reshape(row_count, model_width)
    slot_weights = weights.reshape(row_count, 1)

    gate_pre = jnp.dot(x_rows, w_gate[0], preferred_element_type=f32)
    up_pre = jnp.dot(x_rows, w_up[0], preferred_element_type=f32)
    plain_grad = jnp.einsum("rd,fd->rf", dy_rows, w_down[0], preferred_element_type=f32)
    glu = jnp.minimum(gate_pre, clamp_limit)
    linear = jnp.clip(up_pre, -clamp_limit, clamp_limit)
    sigma = jax.nn.sigmoid(sigmoid_slope * glu)
    active = glu * sigma
    hidden = active * (linear + 1.0)
    product = jnp.sum(hidden * plain_grad, axis=1)
    hidden_grad = plain_grad * slot_weights
    slope_term = sigma + sigmoid_slope * active * (1.0 - sigma)
    gate_pre_grad = jnp.where(
        gate_pre < clamp_limit, hidden_grad * (linear + 1.0) * slope_term, 0.0
    ).astype(bf16)
    up_pre_grad = jnp.where(jnp.abs(up_pre) < clamp_limit, hidden_grad * active, 0.0).astype(bf16)
    hidden = (hidden * slot_weights).astype(bf16)

    row_term = jnp.einsum("rf,df->rd", gate_pre_grad, w_gate[0], preferred_element_type=f32)
    row_term = row_term + jnp.einsum(
        "rf,df->rd", up_pre_grad, w_up[0], preferred_element_type=f32
    )
    row_term = row_term.astype(bf16).reshape(ep_count, capacity, model_width)
    back_rows, back_products = combine(
        row_term, product.reshape(ep_count, 1, capacity), width
    )
    gate_grads = jnp.einsum("rd,rf->df", x_rows, gate_pre_grad, preferred_element_type=f32)
    up_grads = jnp.einsum("rd,rf->df", x_rows, up_pre_grad, preferred_element_type=f32)
    down_grads = jnp.einsum("rf,rd->fd", hidden, dy_rows, preferred_element_type=f32)
    token_grad = jnp.einsum(
        "rt,rw->tw", pick_flat, back_rows.reshape(row_count, width), preferred_element_type=f32
    ).astype(bf16)
    found = jnp.sum(jnp.where(pick, back_products.reshape(experts, capacity, 1), 0.0), axis=1)
    gate_grad = jnp.sum(jnp.where(match, found.T[:, None, :], 0.0), axis=2)
    return (token_grad, gate_grad, gate_grads[None], up_grads[None], down_grads[None])


def solution(mesh):
    return jax.shard_map(
        local,
        mesh=mesh,
        in_specs=(
            P("ep", None),
            P("ep", None),
            P("ep", None),
            P("ep", None),
            P("ep", None, "tp"),
            P("ep", None, "tp"),
            P("ep", "tp", None),
        ),
        out_specs=(
            P("ep", "tp"),
            P("ep", None),
            P("ep", None, "tp"),
            P("ep", None, "tp"),
            P("ep", "tp", None),
        ),
        check_vma=False,
    )
```

```python
import jax
import jax.numpy as jnp
from jax import lax
from jax.experimental import pallas as pl
from jax.experimental.pallas import tpu as pltpu
from jax.sharding import PartitionSpec as P

clamp_limit = 7.0
sigmoid_slope = 1.702
MESH = pl.DeviceIdType.MESH


def partners():
    ep_count = lax.axis_size("ep")
    tp_count = lax.axis_size("tp")
    here = lax.axis_index("ep")
    part = lax.axis_index("tp")
    beside = part + 1 - 2 * (part % 2)
    across = (part + tp_count // 2) % tp_count
    return ep_count, here, part, beside, across


def greet(ep_count, here, part, beside, across):
    barrier = pltpu.get_barrier_semaphore()
    pl.semaphore_signal(barrier, inc=1, device_id=(here, beside), device_id_type=MESH)
    pl.semaphore_signal(barrier, inc=1, device_id=(here, across), device_id_type=MESH)

    def call(j, carry):
        peer = (here + j) % ep_count
        pl.semaphore_signal(barrier, inc=1, device_id=(peer, part), device_id_type=MESH)
        return carry

    lax.fori_loop(1, ep_count, call, 0)
    pl.semaphore_wait(barrier, ep_count + 1)


def remote(src, dst, sent, got, device):
    return pltpu.make_async_remote_copy(
        src_ref=src, dst_ref=dst, send_sem=sent, recv_sem=got, device_id=device, device_id_type=MESH
    )


def dispatch_kernel(
    token_ref, grad_ref, weight_ref, token_rows, grad_rows, weights_out,
    s1, r1, s2, r2, s3, r3, s4, r4, sw, rw, own_sem,
):
    ep_count, here, part, beside, across = partners()
    width = token_ref.shape[2]
    pairs = ((0, token_ref, token_rows), (1, grad_ref, grad_rows))

    def block(rows_ref, source, owner):
        columns = pl.ds(pl.multiple_of(owner * width, width), width)
        return rows_ref.at[source, :, columns]

    greet(ep_count, here, part, beside, across)

    def first(j):
        peer = (here + j) % ep_count
        return [
            remote(send.at[peer], block(rows, here, part), s1.at[i, j], r1.at[i, j], (peer, part))
            for i, send, rows in pairs
        ]

    def first_weight(j):
        peer = (here + j) % ep_count
        return remote(
            weight_ref.at[peer], weights_out.at[here], sw.at[j], rw.at[j], (peer, part)
        )

    def forward(j, owner, sent, got, to):
        source = (here + ep_count - j) % ep_count
        return [
            remote(
                block(rows, source, owner), block(rows, source, owner),
                sent.at[i, j], got.at[i, j], (here, to),
            )
            for i, _, rows in pairs
        ]

    def near(j):
        return forward(j, part, s2, r2, beside)

    def far(j):
        return forward(j, part, s3, r3, across)

    def onward(j):
        return forward(j, across, s4, r4, beside)

    owns = [
        pltpu.make_async_copy(send.at[here], block(rows, here, part), own_sem.at[i])
        for i, send, rows in pairs
    ]
    owns.append(pltpu.make_async_copy(weight_ref.at[here], weights_out.at[here], own_sem.at[2]))
    for copy in owns:
        copy.start()

    def launch(j, carry):
        first_weight(j).start()
        for copy in first(j):
            copy.start()
        return carry

    lax.fori_loop(1, ep_count, launch, 0)
    for copy in owns:
        copy.wait()
    for copy in far(0) + near(0):
        copy.start()

    def pass_on(j, carry):
        @pl.when(j < ep_count)
        def _():
            for i in range(2):
                first(j)[i].wait_recv()
                far(j)[i].start()
                near(j)[i].start()

        @pl.when(j >= 2)
        def _():
            for i in range(2):
                far(j - 2)[i].wait_recv()
                onward(j - 2)[i].start()

        return carry

    lax.fori_loop(1, ep_count + 2, pass_on, 0)

    def finish(j, carry):
        for i in range(2):
            near(j)[i].wait()
            onward(j)[i].wait()
            far(j)[i].wait_send()

        @pl.when(j >= 1)
        def _():
            for copy in first(j):
                copy.wait_send()
            first_weight(j).wait()

        return carry

    lax.fori_loop(0, ep_count, finish, 0)


def dispatch(send_tokens, send_grads, weights, model_width):
    ep_count, capacity, width = send_tokens.shape
    sems = [pltpu.SemaphoreType.DMA((2, ep_count)) for _ in range(8)]
    sems += [pltpu.SemaphoreType.DMA((ep_count,)) for _ in range(2)]
    whole = jax.ShapeDtypeStruct((ep_count, capacity, model_width), jnp.bfloat16)
    return pl.pallas_call(
        dispatch_kernel,
        out_shape=(whole, whole, jax.ShapeDtypeStruct(weights.shape, jnp.float32)),
        in_specs=[pl.BlockSpec(memory_space=pltpu.VMEM)] * 3,
        out_specs=(
            pl.BlockSpec(memory_space=pl.ANY),
            pl.BlockSpec(memory_space=pl.ANY),
            pl.BlockSpec(memory_space=pltpu.VMEM),
        ),
        scratch_shapes=sems + [pltpu.SemaphoreType.DMA((3,))],
        compiler_params=pltpu.CompilerParams(collective_id=0, has_side_effects=True),
    )(send_tokens, send_grads, weights)


def combine_kernel(
    rows_ref, product_ref, back_ref, back_product, near_buf, far_send, far_buf, last_send,
    product_near, product_sum, product_far, product_send,
    s1, r1, s2, r2, s3, r3, sw, rw, small_send, small_recv,
):
    ep_count, here, part, beside, across = partners()
    width = back_ref.shape[2]
    beside_far = (beside + lax.axis_size("tp") // 2) % lax.axis_size("tp")

    def columns(owner):
        return pl.ds(pl.multiple_of(owner * width, width), width)

    greet(ep_count, here, part, beside, across)

    def near(which, j):
        target = (here + j) % ep_count
        owner = beside_far if which == 0 else beside
        return remote(
            rows_ref.at[target, :, columns(owner)], near_buf.at[which, j],
            s1.at[which, j], r1.at[which, j], (here, beside),
        )

    def far(j):
        return remote(far_send.at[j], far_buf.at[j], s2.at[j], r2.at[j], (here, across))

    def last(j):
        peer = (here + j) % ep_count
        return remote(last_send.at[j], back_ref.at[here], s3.at[j], r3.at[j], (peer, part))

    def last_product(j):
        peer = (here + j) % ep_count
        return remote(
            product_send.at[peer], back_product.at[here], sw.at[j], rw.at[j], (peer, part)
        )

    small_near = remote(product_ref, product_near, small_send.at[0], small_recv.at[0], (here, beside))
    small_far = remote(product_sum, product_far, small_send.at[1], small_recv.at[1], (here, across))
    small_near.start()

    def launch(step, carry):
        j = (step + 1) % ep_count
        near(0, j).start()
        near(1, j).start()
        return carry

    lax.fori_loop(0, ep_count, launch, 0)
    small_near.wait_recv()
    product_sum[...] = product_ref[...] + product_near[...]
    small_far.start()

    def middle(step, carry):
        j = (step + 1) % ep_count
        near(0, j).wait_recv()
        target = (here + j) % ep_count
        mine = rows_ref[target, :, columns(across)].astype(jnp.float32)
        far_send[j] = (mine + near_buf[0, j].astype(jnp.float32)).astype(jnp.bfloat16)
        far(j).start()
        return carry

    lax.fori_loop(0, ep_count, middle, 0)
    small_far.wait_recv()
    product_send[...] = product_sum[...] + product_far[...]

    def total(j):
        near(1, j).wait_recv()
        far(j).wait_recv()
        target = (here + j) % ep_count
        mine = rows_ref[target, :, columns(part)].astype(jnp.float32)
        added = mine + near_buf[1, j].astype(jnp.float32) + far_buf[j].astype(jnp.float32)
        return added.astype(jnp.bfloat16)

    def end(j, carry):
        last_send[j] = total(j)
        last(j).start()
        last_product(j).start()
        return carry

    lax.fori_loop(1, ep_count, end, 0)
    back_ref[here] = total(0)
    back_product[here] = product_send[here]

    small_near.wait_send()
    small_far.wait_send()

    def finish(j, carry):
        near(0, j).wait_send()
        near(1, j).wait_send()
        far(j).wait_send()

        @pl.when(j >= 1)
        def _():
            last(j).wait()
            last_product(j).wait()

        return carry

    lax.fori_loop(0, ep_count, finish, 0)


def combine(rows, products, width):
    ep_count, capacity, _ = rows.shape
    one = (ep_count, capacity, width)
    small = pltpu.VMEM(products.shape, jnp.float32)
    dma = pltpu.SemaphoreType.DMA
    return pl.pallas_call(
        combine_kernel,
        out_shape=(
            jax.ShapeDtypeStruct(one, jnp.bfloat16),
            jax.ShapeDtypeStruct(products.shape, jnp.float32),
        ),
        in_specs=[pl.BlockSpec(memory_space=pltpu.VMEM)] * 2,
        out_specs=(pl.BlockSpec(memory_space=pltpu.VMEM),) * 2,
        scratch_shapes=[
            pltpu.VMEM((2,) + one, jnp.bfloat16),
            pltpu.VMEM(one, jnp.bfloat16),
            pltpu.VMEM(one, jnp.bfloat16),
            pltpu.VMEM(one, jnp.bfloat16),
            small, small, small, small,
            dma((2, ep_count)), dma((2, ep_count)),
            dma((ep_count,)), dma((ep_count,)), dma((ep_count,)), dma((ep_count,)),
            dma((ep_count,)), dma((ep_count,)), dma((2,)), dma((2,)),
        ],
        compiler_params=pltpu.CompilerParams(
            collective_id=1, has_side_effects=True, vmem_limit_bytes=48 * 1024 * 1024
        ),
    )(rows, products)


def local(tokens, routes, gate_weights, out_grad, w_gate, w_up, w_down):
    f32, bf16 = jnp.float32, jnp.bfloat16
    ep_count = lax.axis_size("ep")
    tp_count = lax.axis_size("tp")
    part = lax.axis_index("tp")
    token_count, model_width = tokens.shape
    top_count = routes.shape[1]
    experts = ep_count * w_gate.shape[0]
    capacity = token_count * top_count * 5 // (4 * experts)
    width = model_width // tp_count

    match = routes[:, :, None] == jnp.arange(experts, dtype=jnp.int32)[None, None, :]
    named = jnp.any(match, axis=1)
    before = jnp.arange(token_count)[:, None] > jnp.arange(token_count)[None, :]
    rank = jnp.dot(before.astype(bf16), named.astype(bf16), preferred_element_type=f32)
    rank = jnp.where(named, rank.astype(jnp.int32), -1)
    pick = rank.T[:, None, :] == jnp.arange(capacity, dtype=jnp.int32)[None, :, None]
    pick_flat = pick.reshape(experts * capacity, token_count).astype(bf16)
    weight_of = jnp.sum(jnp.where(match, gate_weights[:, :, None], 0.0), axis=1)
    send_weights = jnp.sum(jnp.where(pick, weight_of.T[:, None, :], 0.0), axis=2)
    sends = []
    for array in (tokens, out_grad):
        own = lax.dynamic_slice_in_dim(array, part * width, width, 1)
        picked = jnp.dot(pick_flat, own, preferred_element_type=f32).astype(bf16)
        sends.append(picked.reshape(experts, capacity, width))

    rows, grads, weights = dispatch(*sends, send_weights[:, None, :], model_width)
    row_count = ep_count * capacity
    x_rows = rows.reshape(row_count, model_width)
    dy_rows = grads.reshape(row_count, model_width)
    slot_weights = weights.reshape(row_count, 1)

    gate_pre = jnp.dot(x_rows, w_gate[0], preferred_element_type=f32)
    up_pre = jnp.dot(x_rows, w_up[0], preferred_element_type=f32)
    plain_grad = jnp.einsum("rd,fd->rf", dy_rows, w_down[0], preferred_element_type=f32)
    glu = jnp.minimum(gate_pre, clamp_limit)
    linear = jnp.clip(up_pre, -clamp_limit, clamp_limit)
    sigma = jax.nn.sigmoid(sigmoid_slope * glu)
    active = glu * sigma
    hidden = active * (linear + 1.0)
    product = jnp.sum(hidden * plain_grad, axis=1)
    hidden_grad = plain_grad * slot_weights
    slope_term = sigma + sigmoid_slope * active * (1.0 - sigma)
    gate_pre_grad = jnp.where(
        gate_pre < clamp_limit, hidden_grad * (linear + 1.0) * slope_term, 0.0
    ).astype(bf16)
    up_pre_grad = jnp.where(jnp.abs(up_pre) < clamp_limit, hidden_grad * active, 0.0).astype(bf16)
    hidden = (hidden * slot_weights).astype(bf16)

    row_term = jnp.einsum("rf,df->rd", gate_pre_grad, w_gate[0], preferred_element_type=f32)
    row_term = row_term + jnp.einsum(
        "rf,df->rd", up_pre_grad, w_up[0], preferred_element_type=f32
    )
    row_term = row_term.astype(bf16).reshape(ep_count, capacity, model_width)
    back_rows, back_products = combine(
        row_term, product.reshape(ep_count, 1, capacity), width
    )
    gate_grads = jnp.einsum("rd,rf->df", x_rows, gate_pre_grad, preferred_element_type=f32)
    up_grads = jnp.einsum("rd,rf->df", x_rows, up_pre_grad, preferred_element_type=f32)
    down_grads = jnp.einsum("rf,rd->fd", hidden, dy_rows, preferred_element_type=f32)
    token_grad = jnp.einsum(
        "rt,rw->tw", pick_flat, back_rows.reshape(row_count, width), preferred_element_type=f32
    ).astype(bf16)
    found = jnp.sum(jnp.where(pick, back_products.reshape(experts, capacity, 1), 0.0), axis=1)
    gate_grad = jnp.sum(jnp.where(match, found.T[:, None, :], 0.0), axis=2)
    return (token_grad, gate_grad, gate_grads[None], up_grads[None], down_grads[None])


def solution(mesh):
    return jax.shard_map(
        local,
        mesh=mesh,
        in_specs=(
            P("ep", None),
            P("ep", None),
            P("ep", None),
            P("ep", None),
            P("ep", None, "tp"),
            P("ep", None, "tp"),
            P("ep", "tp", None),
        ),
        out_specs=(
            P("ep", "tp"),
            P("ep", None),
            P("ep", None, "tp"),
            P("ep", None, "tp"),
            P("ep", "tp", None),
        ),
        check_vma=False,
    )
```
